256 devices in a mesh: ep: 64 (over z, x, core), tp: 4 (over y).
Axes of the slice: x: 4, y: 4, z: 8, core: 2. Of those that a mesh axis runs over, the one named last changes fastest.
Arguments:
- query_latent: bfloat16 [16384, 512], P(('ep', 'tp')), may hold values from -6 to 6
- key_latent: bfloat16 [16384, 256], P(('ep', 'tp')), may hold values from -6 to 6
- rotary_key: bfloat16 [16384, 32], P(('ep', 'tp')), may hold values from -140 to 140
- query_gain: float32 [512], replicated, may hold values from 0.1 to 1.9
- latent_gain: float32 [256], replicated, may hold values from 0.1 to 1.9
- query_content: bfloat16 [512, 512], replicated, may hold values from -0.625 to 0.625
- query_rotary: bfloat16 [512, 256], replicated, may hold values from -0.625 to 0.625
- key_content: bfloat16 [256, 512], replicated, may hold values from -0.375 to 0.375
- value_weight: bfloat16 [256, 512], replicated, may hold values from -0.375 to 0.375
- output_weight: bfloat16 [512, 2048], P('tp'), may hold values from -1 to 1
- expert_input: bfloat16 [16384, 2048], P(('ep', 'tp')), may hold values from -6 to 6
- norm_gain: float32 [2048], replicated, may hold values from 0.1 to 1.9
- routes: int32 [16384, 2], P(('ep', 'tp')), may hold values from 0 to 127, all different within a row; in each aligned block of 64 rows (0 to 63, 64 to 127, ...) at most 2 rows name the same one
- route_weight: float32 [16384, 2], P(('ep', 'tp')), may hold values from 0.25 to 2
- expert_gate: bfloat16 [128, 2048, 1024], P('ep', None, 'tp'), may hold values from -0.125 to 0.125
- expert_up: bfloat16 [128, 2048, 1024], P('ep', None, 'tp'), may hold values from -0.125 to 0.125
- expert_down: bfloat16 [128, 1024, 2048], P('ep', 'tp'), may hold values from -0.1875 to 0.1875
- shared_gate: bfloat16 [2048, 1024], P(None, 'tp'), may hold values from -0.125 to 0.125
- shared_up: bfloat16 [2048, 1024], P(None, 'tp'), may hold values from -0.125 to 0.125
- shared_down: bfloat16 [1024, 2048], P('tp'), may hold values from -0.1875 to 0.1875
Outputs:
- mixer_out: bfloat16 [16384, 2048], P(('ep', 'tp'))
- expert_out: bfloat16 [16384, 2048], P(('ep', 'tp'))
The draws below stay inside these ranges and needn't reach their ends.
Inputs may be any that keep to these rules, and one draw needn't show every extreme that they name: `routes`: each row names 2 different experts. Within the rows of one device (aligned blocks of 64 rows) no expert is named by more than 2 rows, and in every draw some expert is named by exactly 2 rows of some device.
All inputs are finite; a program needn't handle non-finite values.
Results may differ from the reference program's by a relative error of at most 0.013.
The reference program's roundings to bfloat16 on the way count: a program that leaves them out, or rounds other values in their place, can miss the bound.
Values may be sent and summed in bfloat16 or wider, within the bound.
A program may use at most 128 MiB of HBM per device.

```python
import math
from functools import partial
import jax
import jax.numpy as jnp
import numpy as np
from jax import lax

D = 2048
HEADS = 8
CONTENT = 64
ROTARY = 32
VALUE = 64
QUERY_RANK = 512
KEY_RANK = 256
EXPERT_WIDTH = 1024
SHARED_WIDTH = 1024
TOPK = 2
TOK_B = 64
EXPERTS = 128
CAPACITY = 2
TOKENS_A = 16384
TOKENS_B = 16384
N_EP = 64
N_TP = 4


def draw_rotary_key(key, part):
    normal_part = jnp.clip(jax.random.normal(jax.random.fold_in(key, 11), (TOKENS_A, ROTARY), jnp.float32), -6.0, 6.0)
    entries = normal_part
    return entries.astype(jnp.bfloat16)


def block_levels(rng, dims, shards, smallest, top_value):
    level = 1.0
    for dim, blocks in shards:
        draws = jax.random.uniform(jax.random.fold_in(jax.random.fold_in(rng, 6), dim), (blocks,), jnp.float32, smallest / len(shards), top_value / len(shards))
        level = level * jnp.repeat(jnp.exp(draws), dims[dim] // blocks).reshape((-1,) + (1,) * (len(dims) - 1 - dim))
    return level


def deal_out(rng, own, number, rows, amount, top, limit, slope):
    sequence = jax.random.permutation(rng, amount)
    crowded, ordinary = load_shares(amount, rows * top, limit, slope, True), load_shares(amount, rows * top, limit, slope, False)
    places = jnp.arange(amount)

    def named(sizes, turn):
        used = int((sizes > 0).sum())
        fixed = max(1, used // 4)
        moved = fixed + (places - fixed + turn * (used - fixed)) % max(1, amount - fixed)
        return jnp.zeros((amount,), jnp.int32).at[sequence[jnp.where(places < fixed, places, moved)]].set(jnp.asarray(sizes, jnp.int32))

    sizes = jnp.where(number % 4 == 0, named(crowded, number // 4), named(ordinary, number - number // 4 - 1))
    mixed = jax.random.permutation(jax.random.fold_in(own, 3), amount)
    source_of, taker = mixed[0:amount // 2 * 2:2], mixed[1:amount // 2 * 2:2]
    slack = jnp.minimum(sizes[source_of] - 1, limit - sizes[taker]) // 2
    slack = jnp.where((source_of == sequence[0]) | (taker == sequence[0]) | (sizes[taker] == 0), 0, jnp.maximum(slack, 0))
    moved = jax.random.randint(jax.random.fold_in(own, 4), (amount // 2,), 0, 1 << 20) % (slack + 1)
    sizes = sizes.at[source_of].add(-moved).at[taker].add(moved)
    labels = jnp.searchsorted(jnp.cumsum(sizes), jnp.arange(rows * top), side="right").astype(jnp.int32)
    grid = labels.reshape(top, rows).T
    grid = grid[jax.random.permutation(jax.random.fold_in(own, 1), rows)]
    turn = jax.random.randint(jax.random.fold_in(own, 2), (rows, 1), 0, top)
    return jnp.take_along_axis(grid, (jnp.arange(top)[None, :] + turn) % top, axis=1)


def load_shares(number_of, total, limit, skew, full):
    portions = [(1 << 20) // math.isqrt(rank ** skew) + 1 for rank in range(1, number_of + 1)]
    largest = limit if full else min(limit, max(-(-total // number_of), total * portions[0] // sum(portions)))
    least = 1 if total - largest >= number_of - 1 else 0
    holding, surplus = [largest] + [least] * (number_of - 1), total - largest - least * (number_of - 1)
    while surplus > 0:
        movable = [i for i in range(1, number_of) if holding[i] < largest] or [i for i in range(1, number_of) if holding[i] < limit]
        mass, budget = sum([portions[i] for i in movable]), surplus
        for i in movable:
            addition = min(limit - holding[i], max(1, budget * portions[i] // mass), surplus)
            holding[i] = holding[i] + addition
            surplus = surplus - addition
    return np.array(holding)


def gaussian(own_key, dims, scale, reach, pieces=(), held_as=jnp.bfloat16):
    values = jax.random.normal(own_key, dims, jnp.float32) * scale
    if len(pieces) > 0:
        values = block_levels(own_key, dims, pieces, -0.22, 0.18) * values
    return jnp.clip(values, min=-reach, max=reach).astype(held_as)


def setup_inputs(seed: int = 0) -> dict:
    streams_of = jax.random.split(jax.random.key(seed), 21)
    query_latent = gaussian(streams_of[0], (TOKENS_A, QUERY_RANK), 1.0, 6.0, ((0, 256),))
    key_latent = gaussian(streams_of[1], (TOKENS_A, KEY_RANK), 1.0, 6.0, ((0, 256),))
    rotary_key = draw_rotary_key(jax.random.fold_in(streams_of[20], 71), 0)
    query_gain = jnp.clip(1.0 + 0.18 * jax.random.normal(streams_of[3], (QUERY_RANK,), jnp.float32), 0.1, 1.9)
    latent_gain = jnp.clip(1.0 + 0.18 * jax.random.normal(streams_of[4], (KEY_RANK,), jnp.float32), 0.1, 1.9)
    query_content = gaussian(streams_of[5], (QUERY_RANK, HEADS * CONTENT), (QUERY_RANK // 6) ** -0.5, 0.625)
    query_rotary = gaussian(streams_of[6], (QUERY_RANK, HEADS * ROTARY), (QUERY_RANK // 6) ** -0.5, 0.625)
    key_content = gaussian(streams_of[7], (KEY_RANK, HEADS * CONTENT), KEY_RANK ** -0.5, 0.375)
    value_weight = gaussian(streams_of[8], (KEY_RANK, HEADS * VALUE), KEY_RANK ** -0.5, 0.375)
    output_weight = gaussian(streams_of[9], (HEADS * VALUE, D), (HEADS * VALUE // 16) ** -0.5, 1.0, ((0, 4),))
    expert_input = gaussian(streams_of[10], (TOKENS_B, D), 1.0, 6.0, ((0, 256),))
    norm_gain = jnp.clip(1.0 + 0.18 * jax.random.normal(streams_of[11], (D,), jnp.float32), 0.1, 1.9)
    routes_keys = jax.random.split(jax.random.fold_in(streams_of[12], 1), TOKENS_B // TOK_B)
    routes_turns = jax.random.permutation(jax.random.fold_in(streams_of[12], 3), TOKENS_B // TOK_B)
    routes = jax.vmap(lambda own, number: deal_out(jax.random.fold_in(streams_of[12], 2), own, number, TOK_B, EXPERTS, TOPK, CAPACITY, 1))(routes_keys, routes_turns).reshape((TOKENS_B, TOPK))
    route_weight = jnp.clip(0.25 + 1.75 * jax.random.uniform(streams_of[13], (TOKENS_B, TOPK), jnp.float32) ** block_levels(streams_of[13], (TOKENS_B, TOPK), ((0, 256),), -0.2, 0.2), 0.25, 2.0)
    expert_gate = gaussian(streams_of[14], (EXPERTS, D, EXPERT_WIDTH), D ** -0.5, 0.125, ((0, 64), (2, 4)))
    expert_up = gaussian(streams_of[15], (EXPERTS, D, EXPERT_WIDTH), D ** -0.5, 0.125, ((0, 64), (2, 4)))
    expert_down = gaussian(streams_of[16], (EXPERTS, EXPERT_WIDTH, D), EXPERT_WIDTH ** -0.5, 0.1875, ((0, 64), (1, 4)))
    shared_gate = gaussian(streams_of[17], (D, SHARED_WIDTH), D ** -0.5, 0.125, ((1, 4),))
    shared_up = gaussian(streams_of[18], (D, SHARED_WIDTH), D ** -0.5, 0.125, ((1, 4),))
    shared_down = gaussian(streams_of[19], (SHARED_WIDTH, D), SHARED_WIDTH ** -0.5, 0.1875, ((0, 4),))
    return {"query_latent": query_latent, "key_latent": key_latent, "rotary_key": rotary_key, "query_gain": query_gain, "latent_gain": latent_gain, "query_content": query_content, "query_rotary": query_rotary, "key_content": key_content, "value_weight": value_weight, "output_weight": output_weight, "expert_input": expert_input, "norm_gain": norm_gain, "routes": routes, "route_weight": route_weight, "expert_gate": expert_gate, "expert_up": expert_up, "expert_down": expert_down, "shared_gate": shared_gate, "shared_up": shared_up, "shared_down": shared_down}


norm_eps = 1e-06
rope_base = 10000.0

def rms_rows(entries, gain_row):
    widened = entries.astype(jnp.float32)
    return widened * lax.rsqrt(lax.optimization_barrier(jnp.mean(widened * widened, -1, keepdims=True)) + norm_eps) * gain_row.astype(jnp.float32)

def turn_pairs(entries, positions):
    width_full = entries.shape[-1]
    frequency = rope_base ** (-jnp.arange(width_full // 2, dtype=jnp.float32) * 2.0 / width_full)
    angles = positions.astype(jnp.float32)[:, None] * frequency[None, :]
    cosine = jnp.cos(angles)[:, None, :]
    sine_part = jnp.sin(angles)[:, None, :]
    even_part = entries[..., 0::2]
    odd_part = entries[..., 1::2]
    joined = jnp.stack([even_part * cosine - odd_part * sine_part, even_part * sine_part + odd_part * cosine], -1)
    return joined.reshape(entries.shape)

def feed_forward(row_block, gate_weight, up_weight, down_weight, groups):
    gated = jnp.dot(row_block, gate_weight, preferred_element_type=jnp.float32)
    lifted = jnp.dot(row_block, up_weight, preferred_element_type=jnp.float32)
    hidden = (jax.nn.silu(gated) * lifted).astype(jnp.bfloat16)
    group_width = hidden.shape[1] // groups
    running = jnp.zeros((row_block.shape[0], down_weight.shape[1]), jnp.float32)
    for group_index in range(groups):
        product = jnp.dot(hidden[:, group_index * group_width:(group_index + 1) * group_width], down_weight[group_index * group_width:(group_index + 1) * group_width], preferred_element_type=jnp.float32)
        running = running + lax.optimization_barrier(product.astype(jnp.bfloat16)).astype(jnp.float32)
    return running

def attend_queries(query_blocks, key_wide, turn_wide, value_wide):
    query_part, query_turn = query_blocks
    score_scale = (CONTENT + ROTARY) ** (-0.5)
    scores = jnp.einsum('qhc,khc->qhk', query_part.astype(jnp.float32), key_wide)
    scores = scores + jnp.einsum('qhr,kr->qhk', query_turn.astype(jnp.float32), turn_wide)
    scores = scores * score_scale
    weights = jnp.exp(scores - lax.optimization_barrier(jnp.max(scores, -1, keepdims=True)))
    denominator = lax.optimization_barrier(jnp.sum(weights, -1))
    rounded = lax.optimization_barrier(weights.astype(jnp.bfloat16)).astype(jnp.float32)
    numerator = jnp.einsum('qhk,khv->qhv', rounded, value_wide)
    return (numerator / denominator[..., None]).astype(jnp.bfloat16)

def block_slots(route_block):
    flat_routes = route_block.reshape(-1)
    marks = (flat_routes[:, None] == jnp.arange(EXPERTS, dtype=jnp.int32)[None, :]).astype(jnp.int32)
    return lax.optimization_barrier(jnp.sum((jnp.cumsum(marks, 0) - marks) * marks, 1)).reshape(route_block.shape)

def reference(query_latent, key_latent, rotary_key, query_gain, latent_gain, query_content, query_rotary, key_content, value_weight, output_weight, expert_input, norm_gain, routes, route_weight, expert_gate, expert_up, expert_down, shared_gate, shared_up, shared_down):
    row_count = query_latent.shape[0]
    positions = jnp.arange(row_count, dtype=jnp.int32)
    query_normed = rms_rows(query_latent, query_gain).astype(jnp.bfloat16)
    latent_normed = rms_rows(key_latent, latent_gain).astype(jnp.bfloat16)
    query_part = jnp.dot(query_normed, query_content, preferred_element_type=jnp.float32).astype(jnp.bfloat16).reshape(row_count, HEADS, CONTENT)
    query_turn = turn_pairs(jnp.dot(query_normed, query_rotary, preferred_element_type=jnp.float32).reshape(row_count, HEADS, ROTARY), positions).astype(jnp.bfloat16)
    key_turn = turn_pairs(rotary_key.astype(jnp.float32)[:, None, :], positions)[:, 0, :].astype(jnp.bfloat16)
    key_part = jnp.dot(latent_normed, key_content, preferred_element_type=jnp.float32).astype(jnp.bfloat16).reshape(row_count, HEADS, CONTENT)
    value_rows = jnp.dot(latent_normed, value_weight, preferred_element_type=jnp.float32).astype(jnp.bfloat16).reshape(row_count, HEADS, VALUE)
    query_block = math.gcd(row_count, 256)
    block_count = row_count // query_block
    query_blocks = (query_part.reshape(block_count, query_block, HEADS, CONTENT), query_turn.reshape(block_count, query_block, HEADS, ROTARY))
    attended = lax.map(partial(attend_queries, key_wide=key_part.astype(jnp.float32), turn_wide=key_turn.astype(jnp.float32), value_wide=value_rows.astype(jnp.float32)), query_blocks)
    attended = attended.reshape(row_count, HEADS * VALUE)
    group_width = HEADS * VALUE // N_TP
    mixed = jnp.zeros((row_count, output_weight.shape[1]), jnp.float32)
    for group_index in range(N_TP):
        product = jnp.dot(attended[:, group_index * group_width:(group_index + 1) * group_width], output_weight[group_index * group_width:(group_index + 1) * group_width], preferred_element_type=jnp.float32)
        mixed = mixed + lax.optimization_barrier(product.astype(jnp.bfloat16)).astype(jnp.float32)
    mixer_out = mixed.astype(jnp.bfloat16)
    token_count = expert_input.shape[0]
    device_count = N_EP * N_TP
    per_device = token_count // device_count
    expert_normed = rms_rows(expert_input, norm_gain).astype(jnp.bfloat16)
    slots = jax.vmap(block_slots)(routes.reshape(device_count, per_device, TOPK)).reshape(token_count, TOPK)
    device_of = (jnp.arange(token_count, dtype=jnp.int32) // per_device).astype(jnp.int32)
    token_index = jnp.broadcast_to(jnp.arange(token_count, dtype=jnp.int32)[:, None], (token_count, TOPK))
    table = jnp.full((EXPERTS, device_count, CAPACITY), token_count, jnp.int32)
    table = table.at[routes, jnp.broadcast_to(device_of[:, None], (token_count, TOPK)), slots].set(token_index)
    padded = jnp.concatenate([expert_normed, jnp.zeros((1, expert_normed.shape[1]), jnp.bfloat16)], 0)

    def one_expert(expert_args):
        table_row, gate_weight, up_weight, down_weight = expert_args
        row_block = padded[table_row.reshape(-1)]
        return feed_forward(row_block, gate_weight, up_weight, down_weight, N_TP).astype(jnp.bfloat16)
    results = lax.map(one_expert, (table, expert_gate, expert_up, expert_down))
    flat_index = (routes * (device_count * CAPACITY) + device_of[:, None] * CAPACITY + slots).astype(jnp.int32)
    picked = results.reshape(-1, results.shape[-1])[flat_index.reshape(-1)].reshape(token_count, TOPK, -1)
    routed = lax.optimization_barrier(jnp.sum(route_weight.astype(jnp.float32)[..., None] * picked.astype(jnp.float32), 1))
    shared_sum = feed_forward(expert_normed, shared_gate, shared_up, shared_down, N_TP)
    expert_out = (routed + shared_sum).astype(jnp.bfloat16)
    return (mixer_out, expert_out)
```

```python
import functools
import math

import jax
import jax.numpy as jnp
from jax import lax
from jax.experimental import pallas as pl
from jax.experimental.pallas import tpu as pltpu
from jax.sharding import PartitionSpec as P

MESH = pl.DeviceIdType.MESH
F32 = jnp.float32
BF16 = jnp.bfloat16

HEADS = 8
CONTENT = 64
ROTARY = 32
VALUE = 64
NZ, NX, NC, NY = 8, 4, 2, 4
NXC = NX * NC
ROWS = 64
GROUP = ROWS * NY
D = 2048
CH = 4
CW = D // CH
LAT = 512 + 256 + 128
norm_eps = 1e-06
rope_base = 10000.0
EXP_SCALE = (CONTENT + ROTARY) ** (-0.5) * math.log2(math.e)


def mm(a, b):
    return jnp.dot(a, b, preferred_element_type=F32)


def mm_nt(a, b):
    return lax.dot_general(a, b, (((1,), (1,)), ((), ())), preferred_element_type=F32)


def kernel(
    lat_ref, tok_ref, routes_ref, rw_ref, cos_ref, sin_ref,
    wq_ref, wr_ref, ws_ref, wk_ref, wv_ref, wo_ref,
    gate_hbm, up_hbm, down_hbm, sgate_hbm, sup_hbm, sdown_hbm,
    mix_ref, exp_ref,
    gate_v, up_v, down_v, sgate_v, sup_v, sdown_v, wsem,
    latg, tokg, s1, r1, s2, g, acc, hid, part, rsa, rsb, s3, r3, s4, r4,
    qg, kg, vg, st, osend, ssend, orecv, srecv,
    psh, sha, shb, ssum, pmx, mxa, mxb,
    send_sem, recv_sem,
):
    ep = lax.axis_index("ep")
    y = lax.axis_index("tp")
    z = ep // NXC
    xc = lax.rem(ep, NXC)
    x = xc // NC
    core = lax.rem(xc, NC)
    yp, ym, ya = lax.rem(y + 1, NY), lax.rem(y + NY - 1, NY), lax.rem(y + 2, NY)
    xp, xm, xa = lax.rem(x + 1, NX), lax.rem(x + NX - 1, NX), lax.rem(x + 2, NX)
    xcp, xcm, xca = xp * NC + core, xm * NC + core, xa * NC + core
    mate = x * NC + (1 - core)
    zs = [lax.rem(z + d, NZ) for d in range(NZ)]
    xcs = [lax.rem(xc + d, NXC) for d in range(NXC)]

    used = [0]
    waits = []

    def sems():
        used[0] += 1
        return send_sem.at[used[0] - 1], recv_sem.at[used[0] - 1]

    def remote(src, dst, pair, e, t):
        return pltpu.make_async_remote_copy(
            src_ref=src, dst_ref=dst, send_sem=pair[0], recv_sem=pair[1],
            device_id=(e, t), device_id_type=MESH,
        )

    def send(src, dst, e, t):
        copy = remote(src, dst, sems(), e, t)
        copy.start()
        waits.append(copy.wait_send)
        return copy

    def whole_wait(ref, sem):
        pltpu.make_async_copy(ref, ref, sem).wait()

    loads = []
    for k, (src, dst) in enumerate([
        (gate_hbm, gate_v), (up_hbm, up_v), (down_hbm, down_v),
        (sgate_hbm, sgate_v), (sup_hbm, sup_v), (sdown_hbm, sdown_v),
    ]):
        copy = pltpu.make_async_copy(src, dst, wsem.at[k])
        copy.start()
        loads.append(copy)

    barrier = pltpu.get_barrier_semaphore()
    for d in range(1, NZ):
        pl.semaphore_signal(barrier, inc=1, device_id=(zs[d] * NXC + xc, y), device_id_type=MESH)
    for d in range(1, NXC):
        pl.semaphore_signal(barrier, inc=1, device_id=(z * NXC + xcs[d], y), device_id_type=MESH)
    for t in (yp, ym):
        pl.semaphore_signal(barrier, inc=1, device_id=(ep, t), device_id_type=MESH)
    pl.semaphore_wait(barrier, NZ - 1 + NXC - 1 + 2)

    def gather_start(src, buf):
        return [send(src, buf.at[y], ep, yp), send(src, buf.at[y], ep, ym)]

    def gather_forward(first, buf):
        first[0].wait_recv()
        a = send(buf.at[ym, 0], buf.at[ym, 0], ep, yp)
        first[1].wait_recv()
        b = send(buf.at[yp, 1], buf.at[yp, 1], ep, ym)
        return [a, b]

    def gather_finish(second):
        second[0].wait_recv()
        second[1].wait_recv()

    def reduce_start(parts, far):
        return [
            send(parts.at[ya, 0], far.at[0], ep, yp),
            send(parts.at[ya, 1], far.at[1], ep, ym),
        ]

    def reduce_forward(first, parts, far, near):
        first[0].wait_recv()
        parts[yp, 0] = (parts[yp, 0].astype(F32) + far[0].astype(F32)).astype(BF16)
        a = send(parts.at[yp], near.at[0], ep, yp)
        first[1].wait_recv()
        parts[ym, 1] = (parts[ym, 1].astype(F32) + far[1].astype(F32)).astype(BF16)
        b = send(parts.at[ym], near.at[1], ep, ym)
        return [a, b]

    def reduce_finish(second, parts, near):
        second[0].wait_recv()
        second[1].wait_recv()
        return parts[y].astype(F32) + near[0].astype(F32) + near[1].astype(F32)

    def exchange_z(c, src, dst):
        pair = sems()
        for d in (4, 3, 5, 2, 6, 1, 7):
            remote(src.at[c, zs[d]], dst.at[c, z], pair, zs[d] * NXC + xc, y).start()
        dst[c, z] = src[c, z]
        waits.append(functools.partial(whole_wait, dst.at[c, pl.ds(0, NZ - 1)], pair[0]))
        return functools.partial(whole_wait, dst.at[c, pl.ds(0, NZ - 1)], pair[1])

    lat_first = gather_start(lat_ref, latg)
    latg[y] = lat_ref[...]

    r0 = routes_ref[0:1, :].astype(F32)
    r1_row = routes_ref[1:2, :].astype(F32)
    i_row = lax.broadcasted_iota(jnp.int32, (ROWS, ROWS), 0)
    i_col = lax.broadcasted_iota(jnp.int32, (ROWS, ROWS), 1)
    eye = i_row == i_col
    before = i_row < i_col

    def as_column(row):
        return jnp.sum(jnp.where(eye, row, 0.0), axis=1, keepdims=True)

    c0, c1 = as_column(r0), as_column(r1_row)

    def target(row):
        hits = jnp.where(before & ((c0 == row) | (c1 == row)), 1.0, 0.0)
        return row * 2.0 + jnp.sum(hits, axis=0, keepdims=True)

    t0, t1 = target(r0), target(r1_row)
    slot = lax.broadcasted_iota(jnp.int32, (256, ROWS), 0).astype(F32)
    picker = jnp.where((slot == t0) | (slot == t1), 1.0, 0.0).astype(BF16)
    slot_t = lax.broadcasted_iota(jnp.int32, (ROWS, 256), 1).astype(F32)
    select = [
        jnp.where(slot_t == as_column(t), 1.0, 0.0).astype(BF16) for t in (t0, t1)
    ]
    share = [as_column(rw_ref[k : k + 1, :]) for k in range(2)]

    z_wait = []
    for c in range(CH):
        tok_c = tok_ref[:, :, c * CW : (c + 1) * CW].reshape(ROWS, CW)
        s1[c] = mm(picker, tok_c).astype(BF16).reshape(NZ, 32, CW)
        z_wait.append(exchange_z(c, s1, r1))
    tok_first = gather_start(tok_ref, tokg)
    tokg[y] = tok_ref[...]

    p_out = lax.broadcasted_iota(jnp.int32, (256, 256), 0)
    p_in = lax.broadcasted_iota(jnp.int32, (256, 256), 1)

    def moved(i):
        return (
            ((i >> 1) & 7) * 32 + (i >> 5) * 4 + ((i >> 4) & 1) * 2 + (i & 1)
        )

    perm = jnp.where(moved(p_out) == p_in, 1.0, 0.0).astype(BF16)
    perm_back = jnp.where(moved(p_in) == p_out, 1.0, 0.0).astype(BF16)

    lat_second = gather_forward(lat_first, latg)
    gather_finish(lat_second)
    lat = latg[...].reshape(GROUP, LAT)
    qn = lat[:, :512]
    ln = lat[:, 512:768]
    kt = lat[:, 768:]
    turned = (mm(qn, wr_ref[...]) * cos_ref[...] + mm(qn, ws_ref[...]) * sin_ref[...]).astype(BF16)
    qq = mm(qn, wq_ref[...]).astype(BF16) + turned
    kk = mm(ln, wk_ref[...]).astype(BF16)
    vt = mm_nt(wv_ref[...], ln).astype(BF16)
    for h in range(2):
        qg[z, h] = qq[:, h * 128 : (h + 1) * 128]
        kg[xc, h] = kk[:, h * 128 : (h + 1) * 128] + kt
        vg[xc, h] = vt[h * 64 : (h + 1) * 64]

    def send_kv(slot_at, halves, e):
        if halves is None:
            return [
                send(kg.at[slot_at], kg.at[slot_at], e, y),
                send(vg.at[slot_at], vg.at[slot_at], e, y),
            ]
        return [
            send(kg.at[slot_at, halves], kg.at[slot_at, halves], e, y),
            send(vg.at[slot_at, halves], vg.at[slot_at, halves], e, y),
        ]

    def wait_kv(copies):
        for copy in copies:
            copy.wait_recv()

    ep_xp, ep_xm, ep_mate = z * NXC + xcp, z * NXC + xcm, z * NXC + mate
    kv_first = [send_kv(xc, None, ep_xp), send_kv(xc, None, ep_xm)]
    kv_mate = [send_kv(xc, None, ep_mate)]
    z_up, z_down = zs[1] * NXC + xc, zs[NZ - 1] * NXC + xc
    q_up = [send(qg.at[z], qg.at[z], z_up, y)]
    q_down = [send(qg.at[z], qg.at[z], z_down, y)]

    def q_forward(step):
        q_up[step - 1].wait_recv()
        if step < 4:
            at = zs[NZ - step]
            q_up.append(send(qg.at[at], qg.at[at], z_up, y))
        if step < 4:
            q_down[step - 1].wait_recv()
            if step < 3:
                at = zs[step]
                q_down.append(send(qg.at[at], qg.at[at], z_down, y))

    def kv_forward():
        wait_kv(kv_first[0])
        second = send_kv(xcm, 0, ep_xp)
        kv_mate.append(send_kv(xcm, None, ep_mate))
        wait_kv(kv_first[1])
        second2 = send_kv(xcp, 1, ep_xm)
        kv_mate.append(send_kv(xcp, None, ep_mate))
        kv_first.append(second)
        kv_first.append(second2)

    def kv_last():
        wait_kv(kv_first[2])
        wait_kv(kv_first[3])
        kv_mate.append(send_kv(xca, None, ep_mate))

    def kv_finish():
        for copies in kv_mate:
            wait_kv(copies)

    o_pair, st_pair = sems(), sems()

    def attend(d):
        at = zs[d]
        for h in range(2):
            qh = qg[at, h]
            peak = None
            for k in range(NXC):
                s = mm_nt(kg[k, h], qh)
                st[h, k] = s
                top = jnp.max(s, axis=0, keepdims=True)
                peak = top if peak is None else jnp.maximum(peak, top)
            total = jnp.zeros((1, GROUP), F32)
            out = jnp.zeros((VALUE, GROUP), F32)
            for k in range(NXC):
                w = jnp.exp2((st[h, k] - peak) * EXP_SCALE)
                total = total + jnp.sum(w, axis=0, keepdims=True)
                out = out + mm(vg[k, h], w.astype(BF16))
            result = (out / total).astype(BF16)
            level = peak * EXP_SCALE + jnp.log2(total)
            if d == 0:
                orecv[z, h * 64 : (h + 1) * 64] = result
                srecv[z, h : h + 1] = level
            else:
                osend[d - 1, h * 64 : (h + 1) * 64] = result
                ssend[d - 1, h : h + 1] = level
        if d:
            e = at * NXC + xc
            remote(osend.at[d - 1], orecv.at[z], o_pair, e, y).start()
            remote(ssend.at[d - 1], srecv.at[z], st_pair, e, y).start()

    def project():
        whole_wait(orecv.at[pl.ds(0, NZ - 1)], o_pair[1])
        whole_wait(srecv.at[pl.ds(0, NZ - 1)], st_pair[1])
        waits.append(functools.partial(whole_wait, osend, o_pair[0]))
        waits.append(functools.partial(whole_wait, ssend, st_pair[0]))
        rows = []
        for h in range(2):
            levels = [srecv[k, h : h + 1] for k in range(NZ)]
            top = functools.reduce(jnp.maximum, levels)
            scaled = [jnp.exp2(v - top) for v in levels]
            total = functools.reduce(lambda a, b: a + b, scaled)
            summed = functools.reduce(
                lambda a, b: a + b,
                [orecv[k, h * 64 : (h + 1) * 64].astype(F32) * scaled[k] for k in range(NZ)],
            )
            rows.append(summed / total)
        attended = jnp.concatenate(rows, axis=0).T.astype(BF16)
        for c in range(CH):
            pmx[:, :, :, c * CW : (c + 1) * CW] = (
                mm(attended, wo_ref[:, c * CW : (c + 1) * CW]).astype(BF16).reshape(NY, 2, 32, CW)
            )
        return reduce_start(pmx, mxa)

    xc_pairs = {}

    def to_expert(c):
        z_wait[c]()
        s2[c] = mm(perm, r1[c].reshape(256, CW)).astype(BF16).reshape(NXC, 32, CW)
        pair = sems()
        for d in (4, 2, 6, 3, 5, 7, 1):
            remote(s2.at[c, xcs[d]], g.at[c, y, xc // 4, lax.rem(xc, 4)], pair, z * NXC + xcs[d], y).start()
        g[c, y, xc // 4, lax.rem(xc, 4)] = s2[c, xc]
        waits.append(functools.partial(whole_wait, s2.at[c, pl.ds(0, NXC - 1)], pair[0]))
        xc_pairs[c] = pair

    g_first, g_second = {}, {}

    def spread(c):
        whole_wait(s2.at[c, pl.ds(0, NXC - 1)], xc_pairs[c][1])
        g_first[c] = [
            send(g.at[c, y], g.at[c, y], ep, yp), send(g.at[c, y], g.at[c, y], ep, ym)
        ]

    def spread_on(c):
        g_second[c] = gather_forward(g_first[c], g.at[c])

    def lift(c):
        gather_finish(g_second[c])
        if c == 0:
            for k in (0, 1):
                loads[k].wait()
        for e in range(2):
            rows = g[c, :, :, :, e * 16 : (e + 1) * 16, :].reshape(512, CW)
            for j, w in enumerate((gate_v, up_v)):
                term = mm(rows, w[e, c * CW : (c + 1) * CW, :])
                acc[e, j] = term if c == 0 else acc[e, j] + term

    def activate():
        loads[2].wait()
        for e in range(2):
            v = acc[e, 0]
            hid[e] = (v / (1.0 + jnp.exp(-v)) * acc[e, 1]).astype(BF16)

    p_first, p_second, x_back, z_back = {}, {}, {}, {}

    def lower(c):
        for e in range(2):
            part[c, :, :, :, e * 16 : (e + 1) * 16, :] = (
                mm(hid[e], down_v[e, :, c * CW : (c + 1) * CW]).astype(BF16).reshape(NY, 2, 4, 16, CW)
            )
        p_first[c] = reduce_start(part.at[c], rsa.at[c])

    def lower_on(c):
        p_second[c] = reduce_forward(p_first[c], part.at[c], rsa.at[c], rsb.at[c])

    def back_x(c):
        s3[c] = reduce_finish(p_second[c], part.at[c], rsb.at[c]).astype(BF16).reshape(NXC, 32, CW)
        pair = sems()
        for d in (4, 2, 6, 3, 5, 7, 1):
            remote(s3.at[c, xcs[d]], r3.at[c, xc], pair, z * NXC + xcs[d], y).start()
        r3[c, xc] = s3[c, xc]
        waits.append(functools.partial(whole_wait, s3.at[c, pl.ds(0, NXC - 1)], pair[0]))
        x_back[c] = pair

    def back_z(c):
        whole_wait(s3.at[c, pl.ds(0, NXC - 1)], x_back[c][1])
        s4[c] = mm(perm_back, r3[c].reshape(256, CW)).astype(BF16).reshape(NZ, 32, CW)
        z_back[c] = exchange_z(c, s4, r4)

    def combine(c):
        z_back[c]()
        rows = r4[c].reshape(256, CW)
        routed = share[0] * mm(select[0], rows) + share[1] * mm(select[1], rows)
        exp_ref[:, c * CW : (c + 1) * CW] = (
            routed + ssum[:, :, c * CW : (c + 1) * CW].reshape(ROWS, CW)
        ).astype(BF16)

    def shared():
        for k in (3, 4, 5):
            loads[k].wait()
        rows = tokg[...].reshape(GROUP, D)
        gated = mm(rows, sgate_v[...])
        lifted = mm(rows, sup_v[...])
        hidden = (gated / (1.0 + jnp.exp(-gated)) * lifted).astype(BF16)
        for c in range(CH):
            psh[:, :, :, c * CW : (c + 1) * CW] = (
                mm(hidden, sdown_v[:, c * CW : (c + 1) * CW]).astype(BF16).reshape(NY, 2, 32, CW)
            )

    to_expert(0)
    kv_forward()
    spread(0)
    q_forward(1)
    to_expert(1)
    kv_last()
    tok_second = gather_forward(tok_first, tokg)
    spread(1)
    spread_on(0)
    q_forward(2)
    to_expert(2)
    kv_finish()
    attend(0)
    spread(2)
    spread_on(1)
    q_forward(3)
    to_expert(3)
    attend(1)
    spread(3)
    lift(0)
    spread_on(2)
    q_forward(4)
    attend(7)
    lift(1)
    spread_on(3)
    gather_finish(tok_second)
    shared()
    sh_first = reduce_start(psh, sha)
    attend(2)
    attend(6)
    lift(2)
    lift(3)
    activate()
    lower(0)
    lower(1)
    lower(2)
    lower(3)
    lower_on(0)
    attend(3)
    lower_on(1)
    sh_second = reduce_forward(sh_first, psh, sha, shb)
    back_x(0)
    lower_on(2)
    attend(5)
    back_z(0)
    back_x(1)
    lower_on(3)
    attend(4)
    ssum[...] = reduce_finish(sh_second, psh, shb)
    back_z(1)
    back_x(2)
    mx_first = project()
    back_z(2)
    back_x(3)
    combine(0)
    mx_second = reduce_forward(mx_first, pmx, mxa, mxb)
    back_z(3)
    combine(1)
    combine(2)
    mix_ref[...] = reduce_finish(mx_second, pmx, mxb).reshape(ROWS, D).astype(BF16)
    combine(3)
    for wait in waits:
        wait()


N_SEMS = 160


def fused(*args):
    vmem = pl.BlockSpec(memory_space=pltpu.VMEM)
    hbm = pl.BlockSpec(memory_space=pl.ANY)
    s = lambda *shape: pltpu.VMEM(shape, BF16)
    f = lambda *shape: pltpu.VMEM(shape, F32)
    return pl.pallas_call(
        kernel,
        out_shape=[jax.ShapeDtypeStruct((ROWS, D), BF16)] * 2,
        in_specs=[vmem] * 12 + [hbm] * 6,
        out_specs=[vmem] * 2,
        scratch_shapes=[
            s(2, D, 256), s(2, D, 256), s(2, 256, D), s(D, 256), s(D, 256), s(256, D),
            pltpu.SemaphoreType.DMA((6,)),
            s(NY, 2, 32, LAT), s(NY, 2, 32, D),
            s(CH, NZ, 32, CW), s(CH, NZ, 32, CW), s(CH, NXC, 32, CW),
            s(CH, NY, 2, 4, 32, CW),
            f(2, 2, 512, 256), s(2, 512, 256),
            s(CH, NY, 2, 4, 32, CW), s(CH, 2, 4, 32, CW), s(CH, 2, 2, 4, 32, CW),
            s(CH, NXC, 32, CW), s(CH, NXC, 32, CW), s(CH, NZ, 32, CW), s(CH, NZ, 32, CW),
            s(NZ, 2, GROUP, 128), s(NXC, 2, GROUP, 128), s(NXC, 2, VALUE, GROUP),
            f(2, NXC, GROUP, GROUP),
            s(NZ - 1, 128, GROUP), f(NZ - 1, 8, GROUP), s(NZ, 128, GROUP), f(NZ, 8, GROUP),
            s(NY, 2, 32, D), s(2, 32, D), s(2, 2, 32, D), f(2, 32, D),
            s(NY, 2, 32, D), s(2, 32, D), s(2, 2, 32, D),
            pltpu.SemaphoreType.DMA((N_SEMS,)), pltpu.SemaphoreType.DMA((N_SEMS,)),
        ],
        compiler_params=pltpu.CompilerParams(
            collective_id=0, has_side_effects=True, vmem_limit_bytes=60 * 1024 * 1024
        ),
        name="fused",
    )(*args)


def rms_rows(entries, gain_row):
    widened = entries.astype(F32)
    return widened * lax.rsqrt(jnp.mean(widened * widened, -1, keepdims=True) + norm_eps) * gain_row


def apart(columns, width, at):
    depth = columns.shape[0]
    blocks = columns.reshape(depth, 2, width)
    return jnp.pad(blocks, ((0, 0), (0, 0), (at, 128 - at - width))).reshape(depth, 256)


def halves(columns):
    blocks = columns.reshape(columns.shape[0], -1, ROTARY // 2, 2)
    even, odd = blocks[..., 0], blocks[..., 1]
    return jnp.concatenate([even, odd], -1), jnp.concatenate([odd, even], -1)


def shards(
    query_latent, key_latent, rotary_key, query_gain, latent_gain, query_content, query_rotary,
    key_content, value_weight, output_weight, expert_input, norm_gain, routes, route_weight,
    expert_gate, expert_up, expert_down, shared_gate, shared_up, shared_down,
):
    y = lax.axis_index("tp")
    start = lax.axis_index("ep") * GROUP
    qn = rms_rows(query_latent, query_gain).astype(BF16)
    ln = rms_rows(key_latent, latent_gain).astype(BF16)
    en = rms_rows(expert_input, norm_gain).astype(BF16)
    frequency = rope_base ** (-jnp.arange(ROTARY // 2, dtype=F32) * 2.0 / ROTARY)
    angles = (start + jnp.arange(GROUP, dtype=jnp.int32)).astype(F32)[:, None] * frequency[None, :]
    cosine, sine = jnp.cos(angles), jnp.sin(angles)
    cos2 = jnp.concatenate([cosine, cosine], -1)
    sin2 = jnp.concatenate([-sine, sine], -1)
    own_cos = lax.dynamic_slice_in_dim(cos2, y * ROWS, ROWS, 0)
    own_sin = lax.dynamic_slice_in_dim(sin2, y * ROWS, ROWS, 0)
    straight, crossed = halves(rotary_key.astype(F32))
    kt = (straight[:, 0] * own_cos + crossed[:, 0] * own_sin).astype(BF16)
    kt = jnp.pad(kt, ((0, 0), (CONTENT, 128 - CONTENT - ROTARY)))
    lat = jnp.concatenate([qn, ln, kt], -1).reshape(2, 32, LAT)
    spread = lambda t: jnp.pad(t, ((0, 0), (CONTENT, 128 - CONTENT - ROTARY)))
    cos_wide = jnp.tile(spread(cos2), (1, 2))
    sin_wide = jnp.tile(spread(sin2), (1, 2))
    cut = lambda w, width: lax.dynamic_slice_in_dim(w, y * 2 * width, 2 * width, 1)
    wq = apart(cut(query_content, CONTENT), CONTENT, 0)
    wr, ws = halves(cut(query_rotary, ROTARY))
    wr, ws = apart(wr, ROTARY, CONTENT), apart(ws, ROTARY, CONTENT)
    wk = apart(cut(key_content, CONTENT), CONTENT, 0)
    wv = cut(value_weight, VALUE).T
    mix, out = fused(
        lat, en.reshape(2, 32, D), routes.T, route_weight.T, cos_wide, sin_wide,
        wq, wr, ws, wk, wv, output_weight,
        expert_gate, expert_up, expert_down, shared_gate, shared_up, shared_down,
    )
    return mix, out


def solution(mesh):
    both = P(("ep", "tp"), None)
    in_specs = (
        both, both, both, P(), P(), P(), P(), P(), P(), P("tp", None), both, P(), both, both,
        P("ep", None, "tp"), P("ep", None, "tp"), P("ep", "tp", None),
        P(None, "tp"), P(None, "tp"), P("tp", None),
    )
    return jax.shard_map(
        shards, mesh=mesh, in_specs=in_specs, out_specs=(both, both), check_vma=False
    )
```

```python
import functools
import math

import jax
import jax.numpy as jnp
import numpy as np
from jax import lax
from jax.experimental import pallas as pl
from jax.experimental.pallas import tpu as pltpu
from jax.sharding import PartitionSpec as P

MESH = pl.DeviceIdType.MESH
F32 = jnp.float32
BF16 = jnp.bfloat16

HEADS = 8
CONTENT = 64
ROTARY = 32
VALUE = 64
NZ, NX, NC, NY = 8, 4, 2, 4
NXC = NX * NC
ROWS = 64
GROUP = ROWS * NY
D = 2048
CH = 8
CW = D // CH
LAT = 512 + 256 + 128
norm_eps = 1e-06
rope_base = 10000.0
EXP_SCALE = (CONTENT + ROTARY) ** (-0.5) * math.log2(math.e)

ORDER = " ".join([
    "X.0 G X.1 Y.0 P X.2 Y.1 X.3 F.0 Y.2 X.4 F.1 Y.3 K X.5 F.2 Y.4 X.6 F.3 Y.5 K2 X.7 F.4 Y.6 T Y.7 F.5 K3",
    "A.0 F.6 S L.0 L.1 Q.1 A.1 F.7 S2 L.2 L.3 L.4 L.5 L.6 L.7 V",
    "W.0 W.1 W.2 A.7 W2.0 W.3 Q.2 A.2 W2.1 W.4 A.6 W2.2 B.0 W.5 Q.3 A.3 W2.3 B.1 Z.0 W.6 A.5",
    "W2.4 B.2 Z.1 W.7 Q.4 A.4 S3 W2.5 B.3 Z.2 C.0 W2.6 B.4 Z.3 C.1 W2.7 M B.5 Z.4 C.2 B.6 Z.5 C.3 B.7 Z.6 M2",
    "C.4 C.5 Z.7 C.6 M3 C.7",
])


def mm(a, b):
    return jnp.dot(a, b, preferred_element_type=F32)


def mm_nt(a, b):
    return lax.dot_general(a, b, (((1,), (1,)), ((), ())), preferred_element_type=F32)


def kernel(
    ql_ref, kl_ref, rk_ref, qgain_ref, lgain_ref, tok_ref, ngain_ref, routes_ref, rw_ref, turn_ref,
    qc_hbm, qr_hbm, kc_hbm, vw_hbm, wo_hbm,
    gate_hbm, up_hbm, down_hbm, sgate_hbm, sup_hbm, sdown_hbm,
    mix_ref, exp_ref,
    gate_v, up_v, down_v, sgate_v, sup_v, sdown_v, qc_v, qr_v, kc_v, vw_v, wo_v, angle, wsem,
    latg, tokg, s1, r1, s2, g, acc, hid, part, rsa, rsb, s3, r3, s4, r4,
    qg, kg, vg, st, osend, ssend, orecv, srecv,
    psh, sha, shb, ssum, pmx, mxa, mxb,
    send_sem, recv_sem,
):
    ep = lax.axis_index("ep")
    y = lax.axis_index("tp")
    z = ep // NXC
    xc = lax.rem(ep, NXC)
    x = xc // NC
    core = lax.rem(xc, NC)
    yp, ym, ya = lax.rem(y + 1, NY), lax.rem(y + NY - 1, NY), lax.rem(y + 2, NY)
    xp, xm, xa = lax.rem(x + 1, NX), lax.rem(x + NX - 1, NX), lax.rem(x + 2, NX)
    xcp, xcm, xca = xp * NC + core, xm * NC + core, xa * NC + core
    mate = x * NC + (1 - core)
    zs = [lax.rem(z + d, NZ) for d in range(NZ)]
    xcs = [lax.rem(xc + d, NXC) for d in range(NXC)]

    used = [0]
    waits = []
    held = {}

    def sems():
        used[0] += 1
        return send_sem.at[used[0] - 1], recv_sem.at[used[0] - 1]

    def remote(src, dst, pair, e, t):
        return pltpu.make_async_remote_copy(
            src_ref=src, dst_ref=dst, send_sem=pair[0], recv_sem=pair[1],
            device_id=(e, t), device_id_type=MESH,
        )

    def send(src, dst, e, t):
        copy = remote(src, dst, sems(), e, t)
        copy.start()
        waits.append(copy.wait_send)
        return copy

    def whole_wait(ref, sem):
        pltpu.make_async_copy(ref, ref, sem).wait()

    barrier = pltpu.get_barrier_semaphore()
    for d in range(1, NZ):
        pl.semaphore_signal(barrier, inc=1, device_id=(zs[d] * NXC + xc, y), device_id_type=MESH)
    for d in range(1, NXC):
        pl.semaphore_signal(barrier, inc=1, device_id=(z * NXC + xcs[d], y), device_id_type=MESH)
    for t in (yp, ym):
        pl.semaphore_signal(barrier, inc=1, device_id=(ep, t), device_id_type=MESH)

    cols = pl.ds(pl.multiple_of(y * 128, 128), 128)
    loads = []
    for k, (src, dst) in enumerate([
        (gate_hbm, gate_v), (up_hbm, up_v), (down_hbm, down_v),
        (sgate_hbm, sgate_v), (sup_hbm, sup_v), (sdown_hbm, sdown_v),
        (qc_hbm.at[:, cols], qc_v), (qr_hbm, qr_v), (kc_hbm.at[:, cols], kc_v),
        (vw_hbm.at[:, cols], vw_v), (wo_hbm, wo_v),
    ]):
        loads.append(pltpu.make_async_copy(src, dst, wsem.at[k]))
    for k in (6, 7, 8, 9, 0, 1, 3, 4, 5, 2, 10):
        loads[k].start()

    def gather_start(src, buf):
        return [send(src, buf.at[y], ep, yp), send(src, buf.at[y], ep, ym)]

    def gather_forward(first, buf):
        first[0].wait_recv()
        a = send(buf.at[ym, 0], buf.at[ym, 0], ep, yp)
        first[1].wait_recv()
        b = send(buf.at[yp, 1], buf.at[yp, 1], ep, ym)
        return [a, b]

    def gather_finish(second):
        second[0].wait_recv()
        second[1].wait_recv()

    def reduce_start(parts, far):
        return [
            send(parts.at[ya, 0], far.at[0], ep, yp),
            send(parts.at[ya, 1], far.at[1], ep, ym),
        ]

    def reduce_forward(first, parts, far, near):
        first[0].wait_recv()
        parts[yp, 0] = (parts[yp, 0].astype(F32) + far[0].astype(F32)).astype(BF16)
        a = send(parts.at[yp], near.at[0], ep, yp)
        first[1].wait_recv()
        parts[ym, 1] = (parts[ym, 1].astype(F32) + far[1].astype(F32)).astype(BF16)
        b = send(parts.at[ym], near.at[1], ep, ym)
        return [a, b]

    def reduce_finish(second, parts, near):
        second[0].wait_recv()
        second[1].wait_recv()
        return parts[y].astype(F32) + near[0].astype(F32) + near[1].astype(F32)

    def exchange_z(c, src, dst):
        pair = sems()
        for d in (4, 3, 5, 2, 6, 1, 7):
            remote(src.at[c, zs[d]], dst.at[c, z], pair, zs[d] * NXC + xc, y).start()
        dst[c, z] = src[c, z]
        waits.append(functools.partial(whole_wait, dst.at[c, pl.ds(0, NZ - 1)], pair[0]))
        return functools.partial(whole_wait, dst.at[c, pl.ds(0, NZ - 1)], pair[1])

    def normed(ref, gain_ref):
        v = ref[...].astype(F32)
        return (v * lax.rsqrt(jnp.mean(v * v, -1, keepdims=True) + norm_eps) * gain_ref[...]).astype(BF16)

    normed_rows = normed(tok_ref, ngain_ref)
    tokg[y] = normed_rows.reshape(2, 32, D)

    r0 = routes_ref[0:1, :].astype(F32)
    r1_row = routes_ref[1:2, :].astype(F32)
    i_row = lax.broadcasted_iota(jnp.int32, (ROWS, ROWS), 0)
    i_col = lax.broadcasted_iota(jnp.int32, (ROWS, ROWS), 1)
    eye = i_row == i_col
    before = i_row < i_col

    def as_column(row):
        return jnp.sum(jnp.where(eye, row, 0.0), axis=1, keepdims=True)

    c0, c1 = as_column(r0), as_column(r1_row)

    def target(row):
        hits = jnp.where(before & ((c0 == row) | (c1 == row)), 1.0, 0.0)
        return row * 2.0 + jnp.sum(hits, axis=0, keepdims=True)

    t0, t1 = target(r0), target(r1_row)
    slot = lax.broadcasted_iota(jnp.int32, (256, ROWS), 0).astype(F32)
    picker = jnp.where((slot == t0) | (slot == t1), 1.0, 0.0).astype(BF16)
    slot_t = lax.broadcasted_iota(jnp.int32, (ROWS, 256), 1).astype(F32)
    select = [
        jnp.where(slot_t == as_column(t), 1.0, 0.0).astype(BF16) for t in (t0, t1)
    ]
    share = [as_column(rw_ref[k : k + 1, :]) for k in range(2)]

    for c in range(CH):
        s1[c] = mm(picker, normed_rows[:, c * CW : (c + 1) * CW]).astype(BF16).reshape(NZ, 32, CW)

    latg[y, :, :, :512] = normed(ql_ref, qgain_ref).reshape(2, 32, 512)
    latg[y, :, :, 512:768] = normed(kl_ref, lgain_ref).reshape(2, 32, 256)
    position = ep * GROUP + lax.broadcasted_iota(jnp.int32, (GROUP, 128), 0)
    angles = position.astype(F32) * turn_ref[0:1, :]
    angle[0] = jnp.cos(angles)
    angle[1] = jnp.sin(angles) * turn_ref[1:2, :]

    def lanes(depth, width):
        return (
            lax.broadcasted_iota(jnp.int32, (depth, width), 0),
            lax.broadcasted_iota(jnp.int32, (depth, width), 1),
        )

    def one_hot(cond):
        return jnp.where(cond, 1.0, 0.0).astype(BF16)

    def rotary_source(lane, flip):
        i = (lane & 127) - CONTENT
        first = (i & 15) * 2
        late = i >> 4
        inside = (i >= 0) & (i < ROTARY)
        return first + ((1 - late) if flip else late), inside

    src, lane = lanes(ROTARY, 128)
    pair = []
    for flip in (False, True):
        entry, inside = rotary_source(lane, flip)
        pick = one_hot((src == entry) & inside)
        pair.append(lax.dot_general(rk_ref[...], pick, (((0,), (0,)), ((), ())), preferred_element_type=F32))
    own = pl.ds(pl.multiple_of(y * ROWS, ROWS), ROWS)
    latg[y, :, :, 768:] = (pair[0] * angle[0, own, :] + pair[1] * angle[1, own, :]).astype(BF16).reshape(2, 32, 128)

    pl.semaphore_wait(barrier, NZ - 1 + NXC - 1 + 2)
    lat_first = gather_start(latg.at[y], latg)
    z_wait = [exchange_z(c, s1, r1) for c in range(CH)]
    tok_first = gather_start(tokg.at[y], tokg)

    p_out = lax.broadcasted_iota(jnp.int32, (256, 256), 0)
    p_in = lax.broadcasted_iota(jnp.int32, (256, 256), 1)

    def moved(i):
        return (
            ((i >> 1) & 7) * 32 + (i >> 5) * 4 + ((i >> 4) & 1) * 2 + (i & 1)
        )

    perm = jnp.where(moved(p_out) == p_in, 1.0, 0.0).astype(BF16)
    perm_back = jnp.where(moved(p_in) == p_out, 1.0, 0.0).astype(BF16)

    def lat_on():
        held["lat"] = gather_forward(lat_first, latg)

    def queries_keys():
        gather_finish(held["lat"])
        for k in (6, 7, 8, 9):
            loads[k].wait()
        lat = latg[...].reshape(GROUP, LAT)
        qn = lat[:, :512]
        ln = lat[:, 512:768]
        kt = lat[:, 768:]
        src, lane = lanes(128, 256)
        spread_out = one_hot((src == (lane >> 7) * CONTENT + (lane & 127)) & ((lane & 127) < CONTENT))
        wq = mm(qc_v[...], spread_out).astype(BF16)
        wk = mm(kc_v[...], spread_out).astype(BF16)
        src, lane = lanes(256, 256)
        wide = []
        for flip in (False, True):
            entry, inside = rotary_source(lane, flip)
            pick = one_hot((src == y * 2 * ROTARY + (lane >> 7) * ROTARY + entry) & inside)
            wide.append(mm(qn, mm(qr_v[...], pick).astype(BF16)))
        cosine = jnp.concatenate([angle[0], angle[0]], axis=1)
        sine = jnp.concatenate([angle[1], angle[1]], axis=1)
        turned = (wide[0] * cosine + wide[1] * sine).astype(BF16)
        qq = mm(qn, wq).astype(BF16) + turned
        kk = mm(ln, wk).astype(BF16)
        vt = mm(ln, vw_v[...]).T.astype(BF16)
        for h in range(2):
            qg[z, h] = qq[:, h * 128 : (h + 1) * 128]
            kg[xc, h] = kk[:, h * 128 : (h + 1) * 128] + kt
            vg[xc, h] = vt[h * 64 : (h + 1) * 64]
        kv_first.extend([send_kv(xc, None, ep_xp), send_kv(xc, None, ep_xm)])
        kv_mate.append(send_kv(xc, None, ep_mate))
        q_up.append(send(qg.at[z], qg.at[z], z_up, y))
        q_down.append(send(qg.at[z], qg.at[z], z_down, y))

    def send_kv(slot_at, halves, e):
        if halves is None:
            return [
                send(kg.at[slot_at], kg.at[slot_at], e, y),
                send(vg.at[slot_at], vg.at[slot_at], e, y),
            ]
        return [
            send(kg.at[slot_at, halves], kg.at[slot_at, halves], e, y),
            send(vg.at[slot_at, halves], vg.at[slot_at, halves], e, y),
        ]

    def wait_kv(copies):
        for copy in copies:
            copy.wait_recv()

    ep_xp, ep_xm, ep_mate = z * NXC + xcp, z * NXC + xcm, z * NXC + mate
    z_up, z_down = zs[1] * NXC + xc, zs[NZ - 1] * NXC + xc
    kv_first, kv_mate, q_up, q_down = [], [], [], []

    def q_forward(step):
        q_up[step - 1].wait_recv()
        if step < 4:
            at = zs[NZ - step]
            q_up.append(send(qg.at[at], qg.at[at], z_up, y))
        if step < 4:
            q_down[step - 1].wait_recv()
            if step < 3:
                at = zs[step]
                q_down.append(send(qg.at[at], qg.at[at], z_down, y))

    def kv_forward():
        wait_kv(kv_first[0])
        second = send_kv(xcm, 0, ep_xp)
        kv_mate.append(send_kv(xcm, None, ep_mate))
        wait_kv(kv_first[1])
        second2 = send_kv(xcp, 1, ep_xm)
        kv_mate.append(send_kv(xcp, None, ep_mate))
        kv_first.append(second)
        kv_first.append(second2)

    def kv_last():
        wait_kv(kv_first[2])
        wait_kv(kv_first[3])
        kv_mate.append(send_kv(xca, None, ep_mate))

    def kv_finish():
        for copies in kv_mate:
            wait_kv(copies)

    o_pair, st_pair = sems(), sems()

    def attend(d):
        at = zs[d]
        for h in range(2):
            qh = qg[at, h]
            peak = None
            for k in range(NXC):
                s = mm_nt(kg[k, h], qh)
                st[h, k] = s
                top = jnp.max(s, axis=0, keepdims=True)
                peak = top if peak is None else jnp.maximum(peak, top)
            total = jnp.zeros((1, GROUP), F32)
            out = jnp.zeros((VALUE, GROUP), F32)
            for k in range(NXC):
                w = jnp.exp2((st[h, k] - peak) * EXP_SCALE)
                total = total + jnp.sum(w, axis=0, keepdims=True)
                out = out + mm(vg[k, h], w.astype(BF16))
            result = (out / total).astype(BF16)
            level = peak * EXP_SCALE + jnp.log2(total)
            if d == 0:
                orecv[z, h * 64 : (h + 1) * 64] = result
                srecv[z, h : h + 1] = level
            else:
                osend[d - 1, h * 64 : (h + 1) * 64] = result
                ssend[d - 1, h : h + 1] = level
        if d:
            e = at * NXC + xc
            remote(osend.at[d - 1], orecv.at[z], o_pair, e, y).start()
            remote(ssend.at[d - 1], srecv.at[z], st_pair, e, y).start()

    def project():
        whole_wait(orecv.at[pl.ds(0, NZ - 1)], o_pair[1])
        whole_wait(srecv.at[pl.ds(0, NZ - 1)], st_pair[1])
        waits.append(functools.partial(whole_wait, osend, o_pair[0]))
        waits.append(functools.partial(whole_wait, ssend, st_pair[0]))
        loads[10].wait()
        rows = []
        for h in range(2):
            levels = [srecv[k, h : h + 1] for k in range(NZ)]
            top = functools.reduce(jnp.maximum, levels)
            scaled = [jnp.exp2(v - top) for v in levels]
            total = functools.reduce(lambda a, b: a + b, scaled)
            summed = functools.reduce(
                lambda a, b: a + b,
                [orecv[k, h * 64 : (h + 1) * 64].astype(F32) * scaled[k] for k in range(NZ)],
            )
            rows.append(summed / total)
        attended = jnp.concatenate(rows, axis=0).T.astype(BF16)
        for c in range(CH):
            pmx[:, :, :, c * CW : (c + 1) * CW] = (
                mm(attended, wo_v[:, c * CW : (c + 1) * CW]).astype(BF16).reshape(NY, 2, 32, CW)
            )
        return reduce_start(pmx, mxa)

    xc_pairs = {}

    def to_expert(c):
        z_wait[c]()
        s2[c] = mm(perm, r1[c].reshape(256, CW)).astype(BF16).reshape(NXC, 32, CW)
        pair = sems()
        for d in (4, 2, 6, 3, 5, 7, 1):
            remote(s2.at[c, xcs[d]], g.at[c, y, xc // 4, lax.rem(xc, 4)], pair, z * NXC + xcs[d], y).start()
        g[c, y, xc // 4, lax.rem(xc, 4)] = s2[c, xc]
        waits.append(functools.partial(whole_wait, s2.at[c, pl.ds(0, NXC - 1)], pair[0]))
        xc_pairs[c] = pair

    g_first, g_second = {}, {}

    def spread(c):
        whole_wait(s2.at[c, pl.ds(0, NXC - 1)], xc_pairs[c][1])
        g_first[c] = [
            send(g.at[c, y], g.at[c, y], ep, yp), send(g.at[c, y], g.at[c, y], ep, ym)
        ]

    def spread_on(c):
        g_second[c] = gather_forward(g_first[c], g.at[c])

    def lift(c):
        gather_finish(g_second[c])
        if c == 0:
            for k in (0, 1):
                loads[k].wait()
        for e in range(2):
            rows = g[c, :, :, :, e * 16 : (e + 1) * 16, :].reshape(512, CW)
            for j, w in enumerate((gate_v, up_v)):
                term = mm(rows, w[e, c * CW : (c + 1) * CW, :])
                acc[e, j] = term if c == 0 else acc[e, j] + term

    def activate():
        loads[2].wait()
        for e in range(2):
            v = acc[e, 0]
            hid[e] = (v / (1.0 + jnp.exp(-v)) * acc[e, 1]).astype(BF16)

    p_first, p_second, x_back, z_back = {}, {}, {}, {}

    def lower(c):
        for e in range(2):
            part[c, :, :, :, e * 16 : (e + 1) * 16, :] = (
                mm(hid[e], down_v[e, :, c * CW : (c + 1) * CW]).astype(BF16).reshape(NY, 2, 4, 16, CW)
            )
        p_first[c] = reduce_start(part.at[c], rsa.at[c])

    def lower_on(c):
        p_second[c] = reduce_forward(p_first[c], part.at[c], rsa.at[c], rsb.at[c])

    def back_x(c):
        s3[c] = reduce_finish(p_second[c], part.at[c], rsb.at[c]).astype(BF16).reshape(NXC, 32, CW)
        pair = sems()
        for d in (4, 2, 6, 3, 5, 7, 1):
            remote(s3.at[c, xcs[d]], r3.at[c, xc], pair, z * NXC + xcs[d], y).start()
        r3[c, xc] = s3[c, xc]
        waits.append(functools.partial(whole_wait, s3.at[c, pl.ds(0, NXC - 1)], pair[0]))
        x_back[c] = pair

    def back_z(c):
        whole_wait(s3.at[c, pl.ds(0, NXC - 1)], x_back[c][1])
        s4[c] = mm(perm_back, r3[c].reshape(256, CW)).astype(BF16).reshape(NZ, 32, CW)
        z_back[c] = exchange_z(c, s4, r4)

    def combine(c):
        z_back[c]()
        rows = r4[c].reshape(256, CW)
        routed = share[0] * mm(select[0], rows) + share[1] * mm(select[1], rows)
        exp_ref[:, c * CW : (c + 1) * CW] = (
            routed + ssum[:, :, c * CW : (c + 1) * CW].reshape(ROWS, CW)
        ).astype(BF16)

    def shared():
        for k in (3, 4, 5):
            loads[k].wait()
        rows = tokg[...].reshape(GROUP, D)
        gated = mm(rows, sgate_v[...])
        lifted = mm(rows, sup_v[...])
        hidden = (gated / (1.0 + jnp.exp(-gated)) * lifted).astype(BF16)
        for c in range(CH):
            psh[:, :, :, c * CW : (c + 1) * CW] = (
                mm(hidden, sdown_v[:, c * CW : (c + 1) * CW]).astype(BF16).reshape(NY, 2, 32, CW)
            )

    def shared_start():
        gather_finish(held["tok"])
        shared()
        held["sh"] = reduce_start(psh, sha)

    def shared_on():
        held["sh"] = reduce_forward(held["sh"], psh, sha, shb)

    def shared_end():
        ssum[...] = reduce_finish(held["sh"], psh, shb)

    def tok_on():
        held["tok"] = gather_forward(tok_first, tokg)

    def mixer():
        held["mx"] = project()

    def mixer_on():
        held["mx"] = reduce_forward(held["mx"], pmx, mxa, mxb)

    def mixer_end():
        mix_ref[...] = reduce_finish(held["mx"], pmx, mxb).reshape(ROWS, D).astype(BF16)

    events = dict(
        X=to_expert, Y=spread, F=spread_on, L=lift, A=attend, Q=q_forward, K=kv_forward,
        K2=kv_last, K3=kv_finish, T=tok_on, S=shared_start, S2=shared_on, S3=shared_end,
        V=activate, W=lower, W2=lower_on, B=back_x, Z=back_z, C=combine,
        M=mixer, M2=mixer_on, M3=mixer_end, G=lat_on, P=queries_keys,
    )
    for item in ORDER.split():
        name, at = (item.split(".") + [None])[:2]
        with jax.named_scope(name if at is None else name + "_" + at):
            events[name](*([] if at is None else [int(at)]))
    assert used[0] <= N_SEMS
    for wait in waits:
        wait()


N_SEMS = 200


def fused(*args):
    vmem = pl.BlockSpec(memory_space=pltpu.VMEM)
    hbm = pl.BlockSpec(memory_space=pl.ANY)
    s = lambda *shape: pltpu.VMEM(shape, BF16)
    f = lambda *shape: pltpu.VMEM(shape, F32)
    return pl.pallas_call(
        kernel,
        out_shape=[jax.ShapeDtypeStruct((ROWS, D), BF16)] * 2,
        in_specs=[vmem] * 10 + [hbm] * 11,
        out_specs=[vmem] * 2,
        scratch_shapes=[
            s(2, D, 256), s(2, D, 256), s(2, 256, D), s(D, 256), s(D, 256), s(256, D),
            s(512, 128), s(512, 256), s(256, 128), s(256, 128), s(128, D), f(2, GROUP, 128),
            pltpu.SemaphoreType.DMA((11,)),
            s(NY, 2, 32, LAT), s(NY, 2, 32, D),
            s(CH, NZ, 32, CW), s(CH, NZ, 32, CW), s(CH, NXC, 32, CW),
            s(CH, NY, 2, 4, 32, CW),
            f(2, 2, 512, 256), s(2, 512, 256),
            s(CH, NY, 2, 4, 32, CW), s(CH, 2, 4, 32, CW), s(CH, 2, 2, 4, 32, CW),
            s(CH, NXC, 32, CW), s(CH, NXC, 32, CW), s(CH, NZ, 32, CW), s(CH, NZ, 32, CW),
            s(NZ, 2, GROUP, 128), s(NXC, 2, GROUP, 128), s(NXC, 2, VALUE, GROUP),
            f(2, NXC, GROUP, GROUP),
            s(NZ - 1, 128, GROUP), f(NZ - 1, 8, GROUP), s(NZ, 128, GROUP), f(NZ, 8, GROUP),
            s(NY, 2, 32, D), s(2, 32, D), s(2, 2, 32, D), f(2, 32, D),
            s(NY, 2, 32, D), s(2, 32, D), s(2, 2, 32, D),
            pltpu.SemaphoreType.DMA((N_SEMS,)), pltpu.SemaphoreType.DMA((N_SEMS,)),
        ],
        compiler_params=pltpu.CompilerParams(
            collective_id=0, has_side_effects=True, vmem_limit_bytes=60 * 1024 * 1024
        ),
        name="fused",
    )(*args)


def turn_table():
    frequency = rope_base ** (-np.arange(ROTARY // 2, dtype=np.float64) * 2.0 / ROTARY)
    table = np.zeros((2, 128), np.float32)
    table[0, CONTENT : CONTENT + ROTARY] = np.tile(frequency, 2)
    table[1, CONTENT : CONTENT + ROTARY] = np.repeat([-1.0, 1.0], ROTARY // 2)
    return jnp.asarray(table)


def shards(
    query_latent, key_latent, rotary_key, query_gain, latent_gain, query_content, query_rotary,
    key_content, value_weight, output_weight, expert_input, norm_gain, routes, route_weight,
    expert_gate, expert_up, expert_down, shared_gate, shared_up, shared_down,
):
    mix, out = fused(
        query_latent, key_latent, rotary_key.T, query_gain[None], latent_gain[None],
        expert_input, norm_gain[None], routes.T, route_weight.T, turn_table(),
        query_content, query_rotary, key_content, value_weight, output_weight,
        expert_gate, expert_up, expert_down, shared_gate, shared_up, shared_down,
    )
    return mix, out


def solution(mesh):
    both = P(("ep", "tp"), None)
    in_specs = (
        both, both, both, P(), P(), P(), P(), P(), P(), P("tp", None), both, P(), both, both,
        P("ep", None, "tp"), P("ep", None, "tp"), P("ep", "tp", None),
        P(None, "tp"), P(None, "tp"), P("tp", None),
    )
    return jax.shard_map(
        shards, mesh=mesh, in_specs=in_specs, out_specs=(both, both), check_vma=False
    )
```

```python
import functools
import math

import jax
import jax.numpy as jnp
import numpy as np
from jax import lax
from jax.experimental import pallas as pl
from jax.experimental.pallas import tpu as pltpu
from jax.sharding import PartitionSpec as P

MESH = pl.DeviceIdType.MESH
F32 = jnp.float32
BF16 = jnp.bfloat16

HEADS = 8
CONTENT = 64
ROTARY = 32
VALUE = 64
NZ, NX, NC, NY = 8, 4, 2, 4
NXC = NX * NC
ROWS = 64
GROUP = ROWS * NY
D = 2048
CH = 8
CW = D // CH
LAT = 512 + 256 + 128
norm_eps = 1e-06
rope_base = 10000.0
EXP_SCALE = (CONTENT + ROTARY) ** (-0.5) * math.log2(math.e)

ORDER = (
    ("G",), ("D",), ("X", 0), ("X", 1), ("P",), ("Y", 0), ("X", 2), ("Y", 1), ("X", 3), ("F", 0),
    ("Y", 2), ("X", 4), ("F", 1), ("Y", 3), ("K",), ("X", 5), ("F", 2), ("Y", 4), ("X", 6), ("F", 3),
    ("Y", 5), ("K2",), ("O",), ("X", 7), ("F", 4), ("Y", 6), ("T",), ("Y", 7), ("F", 5), ("O2",),
    ("K3",), ("A", 0), ("F", 6), ("L", 0), ("L", 1), ("Q", 1), ("A", 1), ("F", 7), ("S",), ("L", 2),
    ("L", 3), ("L", 4), ("L", 5), ("L", 6), ("O3",), ("L", 7), ("V",), ("W", 0), ("W", 1), ("W", 2),
    ("A", 7), ("W2", 0), ("W", 3), ("Q", 2), ("A", 2), ("W2", 1), ("W", 4), ("A", 6), ("W2", 2),
    ("B", 0), ("W", 5), ("Q", 3), ("A", 3), ("W2", 3), ("B", 1), ("Z", 0), ("W", 6), ("O4",), ("A", 5),
    ("W2", 4), ("B", 2), ("Z", 1), ("W", 7), ("Q", 4), ("A", 4), ("W2", 5), ("B", 3), ("Z", 2),
    ("W2", 6), ("B", 4), ("Z", 3), ("W2", 7), ("S2",), ("B", 5), ("Z", 4), ("B", 6), ("B", 7), ("Z", 5),
    ("Z", 6), ("M",), ("Z", 7), ("S3",), ("C", 0), ("C", 1), ("C", 2), ("C", 3), ("C", 4), ("O5",),
    ("M2",), ("C", 5), ("C", 6), ("C", 7),
)


def mm(a, b):
    return jnp.dot(a, b, preferred_element_type=F32)


def mm_nt(a, b):
    return lax.dot_general(a, b, (((1,), (1,)), ((), ())), preferred_element_type=F32)


def kernel(
    ql_ref, kl_ref, rk_ref, qgain_ref, lgain_ref, tok_ref, ngain_ref, routes_ref, rw_ref, turn_ref,
    qc_hbm, qr_hbm, kc_hbm, vw_hbm, wo_hbm,
    gate_hbm, up_hbm, down_hbm, sgate_hbm, sup_hbm, sdown_hbm,
    out_ref,
    gate_v, up_v, down_v, sgate_v, sup_v, sdown_v, qc_v, qr_v, kc_v, vw_v, wog, angle, wsem,
    latg, tokg, s1, r1, s2, g, acc, hid, part, rsa, rsb, s3, r3, s4, r4,
    qg, kg, vg, st, osend, ssend, orecv, srecv,
    psh, sha, shb, ssum, ats, atg,
    send_sem, recv_sem,
):
    ep = lax.axis_index("ep")
    y = lax.axis_index("tp")
    z = ep // NXC
    xc = lax.rem(ep, NXC)
    x = xc // NC
    core = lax.rem(xc, NC)
    yp, ym, ya = lax.rem(y + 1, NY), lax.rem(y + NY - 1, NY), lax.rem(y + 2, NY)
    xp, xm, xa = lax.rem(x + 1, NX), lax.rem(x + NX - 1, NX), lax.rem(x + 2, NX)
    xcp, xcm, xca = xp * NC + core, xm * NC + core, xa * NC + core
    mate = x * NC + (1 - core)
    zs = [lax.rem(z + d, NZ) for d in range(NZ)]
    xcs = [lax.rem(xc + d, NXC) for d in range(NXC)]

    mix_ref, exp_ref = out_ref.at[0], out_ref.at[1]
    used = [0, 0]
    waits = []
    held = {}

    def sems(fresh=True):
        used[0] += fresh
        used[1] += 1
        return send_sem.at[used[0] - 1], recv_sem.at[used[1] - 1]

    def remote(src, dst, pair, e, t):
        return pltpu.make_async_remote_copy(
            src_ref=src, dst_ref=dst, send_sem=pair[0], recv_sem=pair[1],
            device_id=(e, t), device_id_type=MESH,
        )

    def send(src, dst, e, t):
        copy = remote(src, dst, sems(), e, t)
        copy.start()
        waits.append(copy.wait_send)
        return copy

    def send_both(one, other, both):
        copies, pair = [], None
        for src, dst, e, t in (one, other):
            mine = sems(fresh=pair is None)
            pair = mine if pair is None else pair
            copy = remote(src, dst, (pair[0], mine[1]), e, t)
            copy.start()
            copies.append(copy)
        waits.append(functools.partial(whole_wait, both, pair[0]))
        return copies

    def whole_wait(ref, sem):
        pltpu.make_async_copy(ref, ref, sem).wait()

    barrier = pltpu.get_barrier_semaphore()
    for d in range(1, NZ):
        pl.semaphore_signal(barrier, inc=1, device_id=(zs[d] * NXC + xc, y), device_id_type=MESH)
    for d in range(1, NXC):
        pl.semaphore_signal(barrier, inc=1, device_id=(z * NXC + xcs[d], y), device_id_type=MESH)
    for t in (yp, ym, ya):
        pl.semaphore_signal(barrier, inc=1, device_id=(ep, t), device_id_type=MESH)

    cols = pl.ds(pl.multiple_of(y * 128, 128), 128)
    piece = pl.ds(pl.multiple_of(xc * 256, 256), 256)
    loads = []
    for k, (src, dst) in enumerate([
        (gate_hbm, gate_v), (up_hbm, up_v), (down_hbm, down_v),
        (sgate_hbm, sgate_v), (sup_hbm, sup_v), (sdown_hbm, sdown_v),
        (qc_hbm.at[:, cols], qc_v), (qr_hbm, qr_v), (kc_hbm.at[:, cols], kc_v),
        (vw_hbm.at[:, cols], vw_v),
        (wo_hbm.at[0:64, piece], wog.at[xc, y, 0]), (wo_hbm.at[64:128, piece], wog.at[xc, y, 1]),
    ]):
        loads.append(pltpu.make_async_copy(src, dst, wsem.at[k]))
    for k in (10, 11, 6, 7, 8, 9, 0, 1, 3, 4, 5, 2):
        loads[k].start()

    def gather_start(src, buf):
        return send_both((src, buf.at[y], ep, yp), (src, buf.at[y], ep, ym), buf.at[pl.ds(0, 2)])

    def gather_forward(first, buf):
        first[0].wait_recv()
        a = send(buf.at[ym, 0], buf.at[ym, 0], ep, yp)
        first[1].wait_recv()
        b = send(buf.at[yp, 1], buf.at[yp, 1], ep, ym)
        return [a, b]

    def gather_finish(second):
        second[0].wait_recv()
        second[1].wait_recv()

    def reduce_start(parts, far):
        return send_both(
            (parts.at[ya, 0], far.at[0], ep, yp), (parts.at[ya, 1], far.at[1], ep, ym), parts.at[0]
        )

    def reduce_forward(first, parts, far, near):
        first[0].wait_recv()
        parts[yp, 0] = (parts[yp, 0].astype(F32) + far[0].astype(F32)).astype(BF16)
        a = send(parts.at[yp], near.at[0], ep, yp)
        first[1].wait_recv()
        parts[ym, 1] = (parts[ym, 1].astype(F32) + far[1].astype(F32)).astype(BF16)
        b = send(parts.at[ym], near.at[1], ep, ym)
        return [a, b]

    def reduce_finish(second, parts, near):
        second[0].wait_recv()
        second[1].wait_recv()
        return parts[y].astype(F32) + near[0].astype(F32) + near[1].astype(F32)

    def exchange_z(c, src, dst):
        pair = sems()
        for d in (4, 3, 5, 2, 6, 1, 7):
            remote(src.at[c, zs[d]], dst.at[c, z], pair, zs[d] * NXC + xc, y).start()
        dst[c, z] = src[c, z]
        waits.append(functools.partial(whole_wait, dst.at[c, pl.ds(0, NZ - 1)], pair[0]))
        return functools.partial(whole_wait, dst.at[c, pl.ds(0, NZ - 1)], pair[1])

    def normed(ref, gain_ref):
        v = ref[...].astype(F32)
        return (v * lax.rsqrt(jnp.mean(v * v, -1, keepdims=True) + norm_eps) * gain_ref[...]).astype(BF16)

    normed_rows = normed(tok_ref, ngain_ref)
    tokg[y] = normed_rows.reshape(2, 32, D)

    r0 = routes_ref[0:1, :].astype(F32)
    r1_row = routes_ref[1:2, :].astype(F32)
    i_row = lax.broadcasted_iota(jnp.int32, (ROWS, ROWS), 0)
    i_col = lax.broadcasted_iota(jnp.int32, (ROWS, ROWS), 1)
    eye = i_row == i_col
    before = i_row < i_col

    def as_column(row):
        return jnp.sum(jnp.where(eye, row, 0.0), axis=1, keepdims=True)

    c0, c1 = as_column(r0), as_column(r1_row)

    def target(row):
        hits = jnp.where(before & ((c0 == row) | (c1 == row)), 1.0, 0.0)
        return row * 2.0 + jnp.sum(hits, axis=0, keepdims=True)

    t0, t1 = target(r0), target(r1_row)
    slot = lax.broadcasted_iota(jnp.int32, (256, ROWS), 0).astype(F32)
    picker = jnp.where((slot == t0) | (slot == t1), 1.0, 0.0).astype(BF16)
    slot_t = lax.broadcasted_iota(jnp.int32, (ROWS, 256), 1).astype(F32)
    select = [
        jnp.where(slot_t == as_column(t), 1.0, 0.0).astype(BF16) for t in (t0, t1)
    ]
    share = [as_column(rw_ref[k : k + 1, :]) for k in range(2)]

    s1[0] = mm(picker, normed_rows[:, :CW]).astype(BF16).reshape(NZ, 32, CW)
    pl.semaphore_wait(barrier, NZ - 1 + NXC - 1 + NY - 1)
    z_wait = [exchange_z(0, s1, r1)]
    for c in range(1, CH):
        s1[c] = mm(picker, normed_rows[:, c * CW : (c + 1) * CW]).astype(BF16).reshape(NZ, 32, CW)
        z_wait.append(exchange_z(c, s1, r1))
    latg[y, :, :, :512] = normed(ql_ref, qgain_ref).reshape(2, 32, 512)
    latg[y, :, :, 512:768] = normed(kl_ref, lgain_ref).reshape(2, 32, 256)
    position = ep * GROUP + lax.broadcasted_iota(jnp.int32, (GROUP, 128), 0)
    angles = position.astype(F32) * turn_ref[0:1, :]
    angle[0] = jnp.cos(angles)
    angle[1] = jnp.sin(angles) * turn_ref[1:2, :]

    def lanes(depth, width):
        return (
            lax.broadcasted_iota(jnp.int32, (depth, width), 0),
            lax.broadcasted_iota(jnp.int32, (depth, width), 1),
        )

    def one_hot(cond):
        return jnp.where(cond, 1.0, 0.0).astype(BF16)

    def rotary_source(lane, flip):
        i = (lane & 127) - CONTENT
        first = (i & 15) * 2
        late = i >> 4
        inside = (i >= 0) & (i < ROTARY)
        return first + ((1 - late) if flip else late), inside

    src, lane = lanes(ROTARY, 128)
    pair = []
    for flip in (False, True):
        entry, inside = rotary_source(lane, flip)
        pick = one_hot((src == entry) & inside)
        pair.append(lax.dot_general(rk_ref[...], pick, (((0,), (0,)), ((), ())), preferred_element_type=F32))
    own = pl.ds(pl.multiple_of(y * ROWS, ROWS), ROWS)
    latg[y, :, :, 768:] = (pair[0] * angle[0, own, :] + pair[1] * angle[1, own, :]).astype(BF16).reshape(2, 32, 128)

    lat_first = gather_start(latg.at[y], latg)
    loads[10].wait()
    loads[11].wait()
    wo_first = gather_start(wog.at[xc, y], wog.at[xc])

    p_out = lax.broadcasted_iota(jnp.int32, (256, 256), 0)
    p_in = lax.broadcasted_iota(jnp.int32, (256, 256), 1)

    def moved(i):
        return (
            ((i >> 1) & 7) * 32 + (i >> 5) * 4 + ((i >> 4) & 1) * 2 + (i & 1)
        )

    perm = jnp.where(moved(p_out) == p_in, 1.0, 0.0).astype(BF16)
    perm_back = jnp.where(moved(p_in) == p_out, 1.0, 0.0).astype(BF16)

    def lat_on():
        held["lat"] = gather_forward(lat_first, latg)

    def queries_keys():
        gather_finish(held["lat"])
        for k in (6, 7, 8, 9):
            loads[k].wait()
        lat = latg[...].reshape(GROUP, LAT)
        qn = lat[:, :512]
        ln = lat[:, 512:768]
        kt = lat[:, 768:]
        src, lane = lanes(128, 256)
        spread_out = one_hot((src == (lane >> 7) * CONTENT + (lane & 127)) & ((lane & 127) < CONTENT))
        wq = mm(qc_v[...], spread_out).astype(BF16)
        wk = mm(kc_v[...], spread_out).astype(BF16)
        src, lane = lanes(256, 256)
        wide = []
        for flip in (False, True):
            entry, inside = rotary_source(lane, flip)
            pick = one_hot((src == y * 2 * ROTARY + (lane >> 7) * ROTARY + entry) & inside)
            wide.append(mm(qn, mm(qr_v[...], pick).astype(BF16)))
        cosine = jnp.concatenate([angle[0], angle[0]], axis=1)
        sine = jnp.concatenate([angle[1], angle[1]], axis=1)
        turned = (wide[0] * cosine + wide[1] * sine).astype(BF16)
        qq = mm(qn, wq).astype(BF16) + turned
        kk = mm(ln, wk).astype(BF16)
        vt = mm(ln, vw_v[...]).T.astype(BF16)
        for h in range(2):
            qg[z, h] = qq[:, h * 128 : (h + 1) * 128]
            kg[xc, h] = kk[:, h * 128 : (h + 1) * 128] + kt
            vg[xc, h] = vt[h * 64 : (h + 1) * 64]
        kv_first.extend([send_kv(xc, None, ep_xp), send_kv(xc, None, ep_xm)])
        kv_mate.append(send_kv(xc, None, ep_mate))
        q_up.append(send(qg.at[z], qg.at[z], z_up, y))
        q_down.append(send(qg.at[z], qg.at[z], z_down, y))

    def send_kv(slot_at, halves, e):
        if halves is None:
            return [
                send(kg.at[slot_at], kg.at[slot_at], e, y),
                send(vg.at[slot_at], vg.at[slot_at], e, y),
            ]
        return [
            send(kg.at[slot_at, halves], kg.at[slot_at, halves], e, y),
            send(vg.at[slot_at, halves], vg.at[slot_at, halves], e, y),
        ]

    def wait_kv(copies):
        for copy in copies:
            copy.wait_recv()

    ep_xp, ep_xm, ep_mate = z * NXC + xcp, z * NXC + xcm, z * NXC + mate
    z_up, z_down = zs[1] * NXC + xc, zs[NZ - 1] * NXC + xc
    kv_first, kv_mate, q_up, q_down = [], [], [], []

    def q_forward(step):
        q_up[step - 1].wait_recv()
        if step < 4:
            at = zs[NZ - step]
            q_up.append(send(qg.at[at], qg.at[at], z_up, y))
        if step < 4:
            q_down[step - 1].wait_recv()
            if step < 3:
                at = zs[step]
                q_down.append(send(qg.at[at], qg.at[at], z_down, y))

    def kv_forward():
        wait_kv(kv_first[0])
        second = send_kv(xcm, 0, ep_xp)
        kv_mate.append(send_kv(xcm, None, ep_mate))
        wait_kv(kv_first[1])
        second2 = send_kv(xcp, 1, ep_xm)
        kv_mate.append(send_kv(xcp, None, ep_mate))
        kv_first.append(second)
        kv_first.append(second2)

    def kv_last():
        wait_kv(kv_first[2])
        wait_kv(kv_first[3])
        kv_mate.append(send_kv(xca, None, ep_mate))

    def kv_finish():
        for copies in kv_mate:
            wait_kv(copies)

    o_pair, st_pair = sems(), sems()

    def attend(d):
        at = zs[d]
        for h in range(2):
            qh = qg[at, h]
            peak = None
            for k in range(NXC):
                s = mm_nt(kg[k, h], qh)
                st[h, k] = s
                top = jnp.max(s, axis=0, keepdims=True)
                peak = top if peak is None else jnp.maximum(peak, top)
            total = jnp.zeros((1, GROUP), F32)
            out = jnp.zeros((VALUE, GROUP), F32)
            for k in range(NXC):
                w = jnp.exp2((st[h, k] - peak) * EXP_SCALE)
                total = total + jnp.sum(w, axis=0, keepdims=True)
                out = out + mm(vg[k, h], w.astype(BF16))
            result = (out / total).astype(BF16)
            level = peak * EXP_SCALE + jnp.log2(total)
            if d == 0:
                orecv[z, h * 64 : (h + 1) * 64] = result
                srecv[z, h : h + 1] = level
            else:
                osend[d - 1, h * 64 : (h + 1) * 64] = result
                ssend[d - 1, h : h + 1] = level
        if d:
            e = at * NXC + xc
            remote(osend.at[d - 1], orecv.at[z], o_pair, e, y).start()
            remote(ssend.at[d - 1], srecv.at[z], st_pair, e, y).start()

    def project():
        whole_wait(orecv.at[pl.ds(0, NZ - 1)], o_pair[1])
        whole_wait(srecv.at[pl.ds(0, NZ - 1)], st_pair[1])
        waits.append(functools.partial(whole_wait, osend, o_pair[0]))
        waits.append(functools.partial(whole_wait, ssend, st_pair[0]))
        rows = []
        for h in range(2):
            levels = [srecv[k, h : h + 1] for k in range(NZ)]
            top = functools.reduce(jnp.maximum, levels)
            scaled = [jnp.exp2(v - top) for v in levels]
            total = functools.reduce(lambda a, b: a + b, scaled)
            summed = functools.reduce(
                lambda a, b: a + b,
                [orecv[k, h * 64 : (h + 1) * 64].astype(F32) * scaled[k] for k in range(NZ)],
            )
            rows.append(summed / total)
        ats[...] = jnp.concatenate(rows, axis=0).T.astype(BF16).reshape(NY, ROWS, 128)
        held["at"] = [send(ats.at[t], atg.at[y], ep, t) for t in (yp, ym, ya)]
        atg[y] = ats[y]

    def mix():
        for copy in held["at"]:
            copy.wait_recv()
        for c in range(NXC):
            out = jnp.zeros((ROWS, 256), F32)
            for k in range(NY):
                out = out + mm(atg[k], wog[c, k].reshape(128, 256)).astype(BF16).astype(F32)
            mix_ref[:, c * 256 : (c + 1) * 256] = out.astype(BF16)

    def out_on():
        held["wo"] = gather_forward(wo_first, wog.at[xc])

    def out_across():
        gather_finish(held["wo"])
        whole = lambda at, e: send(wog.at[at], wog.at[at], e, y)
        held["wx"] = [whole(xc, ep_xp), whole(xc, ep_xm)]
        held["wm"] = [whole(xc, ep_mate)]

    def out_across_on():
        first, mate_copies = held["wx"], held["wm"]
        low, high = pl.ds(0, 2), pl.ds(2, 2)
        first[0].wait_recv()
        a = send(wog.at[xcm, low], wog.at[xcm, low], ep_xp, y)
        mate_copies.append(send(wog.at[xcm], wog.at[xcm], ep_mate, y))
        first[1].wait_recv()
        b = send(wog.at[xcp, high], wog.at[xcp, high], ep_xm, y)
        mate_copies.append(send(wog.at[xcp], wog.at[xcp], ep_mate, y))
        held["wx"] = [a, b]

    def out_across_last():
        for copy in held["wx"]:
            copy.wait_recv()
        held["wm"].append(send(wog.at[xca], wog.at[xca], ep_mate, y))

    def out_here():
        for copy in held["wm"]:
            copy.wait_recv()

    xc_pairs = {}

    def to_expert(c):
        z_wait[c]()
        s2[c] = mm(perm, r1[c].reshape(256, CW)).astype(BF16).reshape(NXC, 32, CW)
        pair = sems()
        for d in (4, 2, 6, 3, 5, 7, 1):
            remote(s2.at[c, xcs[d]], g.at[c, y, xc // 4, lax.rem(xc, 4)], pair, z * NXC + xcs[d], y).start()
        g[c, y, xc // 4, lax.rem(xc, 4)] = s2[c, xc]
        waits.append(functools.partial(whole_wait, s2.at[c, pl.ds(0, NXC - 1)], pair[0]))
        xc_pairs[c] = pair

    g_first, g_second = {}, {}

    def spread(c):
        whole_wait(s2.at[c, pl.ds(0, NXC - 1)], xc_pairs[c][1])
        g_first[c] = gather_start(g.at[c, y], g.at[c])

    def spread_on(c):
        g_second[c] = gather_forward(g_first[c], g.at[c])

    def lift(c):
        gather_finish(g_second[c])
        if c == 0:
            for k in (0, 1):
                loads[k].wait()
        for e in range(2):
            rows = g[c, :, :, :, e * 16 : (e + 1) * 16, :].reshape(512, CW)
            for j, w in enumerate((gate_v, up_v)):
                term = mm(rows, w[e, c * CW : (c + 1) * CW, :])
                acc[e, j] = term if c == 0 else acc[e, j] + term

    def activate():
        loads[2].wait()
        for e in range(2):
            v = acc[e, 0]
            hid[e] = (v / (1.0 + jnp.exp(-v)) * acc[e, 1]).astype(BF16)

    p_first, p_second, x_back, z_back = {}, {}, {}, {}

    def lower(c):
        for e in range(2):
            part[c, :, :, :, e * 16 : (e + 1) * 16, :] = (
                mm(hid[e], down_v[e, :, c * CW : (c + 1) * CW]).astype(BF16).reshape(NY, 2, 4, 16, CW)
            )
        p_first[c] = reduce_start(part.at[c], rsa.at[c])

    def lower_on(c):
        p_second[c] = reduce_forward(p_first[c], part.at[c], rsa.at[c], rsb.at[c])

    def back_x(c):
        s3[c] = reduce_finish(p_second[c], part.at[c], rsb.at[c]).astype(BF16).reshape(NXC, 32, CW)
        pair = sems()
        for d in (4, 2, 6, 3, 5, 7, 1):
            remote(s3.at[c, xcs[d]], r3.at[c, xc], pair, z * NXC + xcs[d], y).start()
        r3[c, xc] = s3[c, xc]
        waits.append(functools.partial(whole_wait, s3.at[c, pl.ds(0, NXC - 1)], pair[0]))
        x_back[c] = pair

    def back_z(c):
        whole_wait(s3.at[c, pl.ds(0, NXC - 1)], x_back[c][1])
        s4[c] = mm(perm_back, r3[c].reshape(256, CW)).astype(BF16).reshape(NZ, 32, CW)
        z_back[c] = exchange_z(c, s4, r4)

    def combine(c):
        z_back[c]()
        rows = r4[c].reshape(256, CW)
        routed = share[0] * mm(select[0], rows) + share[1] * mm(select[1], rows)
        exp_ref[:, c * CW : (c + 1) * CW] = (
            routed + ssum[:, :, c * CW : (c + 1) * CW].reshape(ROWS, CW)
        ).astype(BF16)

    def shared():
        for k in (3, 4, 5):
            loads[k].wait()
        rows = tokg[...].reshape(GROUP, D)
        gated = mm(rows, sgate_v[...])
        lifted = mm(rows, sup_v[...])
        hidden = (gated / (1.0 + jnp.exp(-gated)) * lifted).astype(BF16)
        for c in range(CH):
            psh[:, :, :, c * CW : (c + 1) * CW] = (
                mm(hidden, sdown_v[:, c * CW : (c + 1) * CW]).astype(BF16).reshape(NY, 2, 32, CW)
            )

    def shared_start():
        gather_finish(held["tok"])
        shared()
        held["sh"] = reduce_start(psh, sha)

    def shared_on():
        held["sh"] = reduce_forward(held["sh"], psh, sha, shb)

    def shared_end():
        ssum[...] = reduce_finish(held["sh"], psh, shb)

    def tok_on():
        held["tok"] = gather_forward(held["tok"], tokg)

    def tok_start():
        held["tok"] = gather_start(tokg.at[y], tokg)

    events = dict(
        X=to_expert, Y=spread, F=spread_on, L=lift, A=attend, Q=q_forward, K=kv_forward,
        K2=kv_last, K3=kv_finish, T=tok_on, S=shared_start, S2=shared_on, S3=shared_end,
        V=activate, W=lower, W2=lower_on, B=back_x, Z=back_z, C=combine,
        M=project, M2=mix, O=out_on, O2=out_across, O3=out_across_on, O4=out_across_last, O5=out_here, G=lat_on, D=tok_start, P=queries_keys,
    )
    for item in ORDER:
        with jax.named_scope("_".join(map(str, item))):
            events[item[0]](*item[1:])
    assert used == [N_SEND, N_RECV], used
    for wait in waits:
        wait()


N_SEND, N_RECV = 128, 148


def fused(*args):
    vmem = pl.BlockSpec(memory_space=pltpu.VMEM)
    hbm = pl.BlockSpec(memory_space=pl.ANY)
    s = lambda *shape: pltpu.VMEM(shape, BF16)
    f = lambda *shape: pltpu.VMEM(shape, F32)
    return pl.pallas_call(
        kernel,
        out_shape=jax.ShapeDtypeStruct((2, ROWS, D), BF16),
        in_specs=[vmem] * 10 + [hbm] * 11,
        out_specs=vmem,
        scratch_shapes=[
            s(2, D, 256), s(2, D, 256), s(2, 256, D), s(D, 256), s(D, 256), s(256, D),
            s(512, 128), s(512, 256), s(256, 128), s(256, 128), s(NXC, NY, 2, 64, 256), f(2, GROUP, 128),
            pltpu.SemaphoreType.DMA((12,)),
            s(NY, 2, 32, LAT), s(NY, 2, 32, D),
            s(CH, NZ, 32, CW), s(CH, NZ, 32, CW), s(CH, NXC, 32, CW),
            s(CH, NY, 2, 4, 32, CW),
            f(2, 2, 512, 256), s(2, 512, 256),
            s(CH, NY, 2, 4, 32, CW), s(CH, 2, 4, 32, CW), s(CH, 2, 2, 4, 32, CW),
            s(CH, NXC, 32, CW), s(CH, NXC, 32, CW), s(CH, NZ, 32, CW), s(CH, NZ, 32, CW),
            s(NZ, 2, GROUP, 128), s(NXC, 2, GROUP, 128), s(NXC, 2, VALUE, GROUP),
            f(2, NXC, GROUP, GROUP),
            s(NZ - 1, 128, GROUP), f(NZ - 1, 8, GROUP), s(NZ, 128, GROUP), f(NZ, 8, GROUP),
            s(NY, 2, 32, D), s(2, 32, D), s(2, 2, 32, D), f(2, 32, D),
            s(NY, ROWS, 128), s(NY, ROWS, 128),
            pltpu.SemaphoreType.DMA((N_SEND,)), pltpu.SemaphoreType.DMA((N_RECV,)),
        ],
        compiler_params=pltpu.CompilerParams(
            collective_id=0, has_side_effects=True, vmem_limit_bytes=60 * 1024 * 1024
        ),
        name="fused",
    )(*args)


def turn_table():
    frequency = rope_base ** (-np.arange(ROTARY // 2, dtype=np.float64) * 2.0 / ROTARY)
    table = np.zeros((2, 128), np.float32)
    table[0, CONTENT : CONTENT + ROTARY] = np.tile(frequency, 2)
    table[1, CONTENT : CONTENT + ROTARY] = np.repeat([-1.0, 1.0], ROTARY // 2)
    return jnp.asarray(table)


def shards(
    query_latent, key_latent, rotary_key, query_gain, latent_gain, query_content, query_rotary,
    key_content, value_weight, output_weight, expert_input, norm_gain, routes, route_weight,
    expert_gate, expert_up, expert_down, shared_gate, shared_up, shared_down,
):
    both = fused(
        query_latent, key_latent, rotary_key.T, query_gain[None], latent_gain[None],
        expert_input, norm_gain[None], routes.T, route_weight.T, turn_table(),
        query_content, query_rotary, key_content, value_weight, output_weight,
        expert_gate, expert_up, expert_down, shared_gate, shared_up, shared_down,
    )
    return both[0].astype(BF16), both[1].astype(BF16)


def solution(mesh):
    both = P(("ep", "tp"), None)
    in_specs = (
        both, both, both, P(), P(), P(), P(), P(), P(), P("tp", None), both, P(), both, both,
        P("ep", None, "tp"), P("ep", None, "tp"), P("ep", "tp", None),
        P(None, "tp"), P(None, "tp"), P("tp", None),
    )
    return jax.shard_map(
        shards, mesh=mesh, in_specs=in_specs, out_specs=(both, both), check_vma=False
    )
```
